32 devices in a mesh: sp: 8 (over z, x), tp: 4 (over y, core).
Axes of the slice: x: 2, y: 2, z: 4, core: 2. Of those that a mesh axis runs over, the one named last changes fastest.
Arguments:
- moe_in: bfloat16 [1536, 2048], P('sp', 'tp'), may hold values from -6 to 6
- cotangent: bfloat16 [1536, 2048], P('sp', 'tp'), may hold values from -6 to 6
- routes: int32 [1536, 2], P('sp'), may hold values from 0 to 7, all different within a row; in each aligned block of 192 rows (0 to 191, 192 to 383, ...) at most 60 rows name the same one
- route_weight: float32 [1536, 2], P('sp'), may hold values from 0.2 to 1
- w_gate: bfloat16 [8, 3584, 2048], P('sp', 'tp'), may hold values from -0.125 to 0.125
- w_up: bfloat16 [8, 3584, 2048], P('sp', 'tp'), may hold values from -0.125 to 0.125
- w_down: bfloat16 [8, 3584, 2048], P('sp', 'tp'), may hold values from -0.09375 to 0.09375
- conv_pre: bfloat16 [1536, 2048], P('sp', 'tp'), may hold values from -6 to 6
- norm_mean: float32 [1536], P('sp'), may hold values from -3 to 3
- norm_rstd: float32 [1536], P('sp'), may hold values from 0.5 to 2
- ln_gain: float32 [2048], P('tp'), may hold values from 0.1 to 1.9
- ln_shift: float32 [2048], P('tp'), may hold values from -3 to 3
- taps: float32 [31, 2048], P(None, 'tp'), may hold values from -1 to 1
- w_proj: bfloat16 [2048, 2048], P('sp', 'tp'), may hold values from -0.125 to 0.125
Outputs:
- grad_up: bfloat16 [8, 3584, 2048], P('sp', 'tp')
- grad_down: bfloat16 [8, 3584, 2048], P('sp', 'tp')
- grad_stream: bfloat16 [1536, 2048], P('sp', 'tp')
- grad_proj: float32 [2048, 2048], P('sp', 'tp')
- grad_conv: bfloat16 [1536, 2048], P('sp', 'tp')
The draws below stay inside these ranges and needn't reach their ends.
Inputs may be any that keep to these rules, and one draw needn't show every extreme that they name: `routes`: each token names 2 different experts. Among the tokens of one index of sp no expert is named more than 60 times, a bound that some block reaches.
All inputs are finite; a program needn't handle non-finite values.
Results may differ from the reference program's by a relative error of at most 0.02.
Values may be sent and summed in bfloat16 or wider, within the bound.
A program may use at most 64 MiB of HBM per device.

```python
import math
import jax
import jax.numpy as jnp
import numpy as np
from jax import lax

D = 2048
FF_E = 3584
KW = 31
TOP = 2
TOK_DEV = 192
EXPERTS = 8
CAP = 60
TOKENS = 1536
N_SP = 8
N_TP = 4


def raised(drawn, key, source, target, shards_of, factor):
    owner, partner = [(jnp.arange(drawn.shape[dim]) // (drawn.shape[dim] // shards_of)).reshape([-1 if axis == dim else 1 for axis in range(drawn.ndim)]) for dim in (source, target)]
    chosen = jax.random.permutation(key, shards_of)[partner]
    strong = (owner == chosen) | (owner == (partner + shards_of // 2) % shards_of)
    return jnp.where(strong, factor * drawn, drawn)


def level_of(stream_key, shape, shards, low, top_value):
    level, own = 1.0, jax.random.fold_in(stream_key, 6)
    for position, shards_of in shards:
        heights = jnp.exp(jax.random.uniform(jax.random.fold_in(own, position), (shards_of,), jnp.float32, low / len(shards), top_value / len(shards)))
        level = level * jnp.repeat(heights, shape[position] // shards_of).reshape([-1 if axis == position else 1 for axis in range(len(shape))])
    return level


def routed_block(stream_key, own, number, rows, count, top, bound, skew):
    sequence = jax.random.permutation(stream_key, count)
    crowded, common = load_shares(count, rows * top, bound, skew, True), load_shares(count, rows * top, bound, skew, False)
    places = jnp.arange(count)

    def named(lengths, turn):
        used = int((lengths > 0).sum())
        fixed = max(1, used // 4)
        passed = fixed + (places - fixed + turn * (used - fixed)) % max(1, count - fixed)
        return jnp.zeros((count,), jnp.int32).at[sequence[jnp.where(places < fixed, places, passed)]].set(jnp.asarray(lengths, jnp.int32))

    lengths = jnp.where(number % 4 == 0, named(crowded, number // 4), named(common, number - number // 4 - 1))
    mixed = jax.random.permutation(jax.random.fold_in(own, 3), count)
    giver, sink = mixed[0:count // 2 * 2:2], mixed[1:count // 2 * 2:2]
    slack = jnp.minimum(lengths[giver] - 1, bound - lengths[sink]) // 2
    slack = jnp.where((giver == sequence[0]) | (sink == sequence[0]) | (lengths[sink] == 0), 0, jnp.maximum(slack, 0))
    passed = jax.random.randint(jax.random.fold_in(own, 4), (count // 2,), 0, 1 << 20) % (slack + 1)
    lengths = lengths.at[giver].add(-passed).at[sink].add(passed)
    members = jnp.searchsorted(jnp.cumsum(lengths), jnp.arange(rows * top), side="right").astype(jnp.int32)
    grid = members.reshape(top, rows).T
    grid = grid[jax.random.permutation(jax.random.fold_in(own, 1), rows)]
    turn = jax.random.randint(jax.random.fold_in(own, 2), (rows, 1), 0, top)
    return jnp.take_along_axis(grid, (jnp.arange(top)[None, :] + turn) % top, axis=1)


def load_shares(amount, total, limit, skew, full):
    weights = [(1 << 20) // math.isqrt(rank ** skew) + 1 for rank in range(1, amount + 1)]
    largest = limit if full else min(limit, max(-(-total // amount), total * weights[0] // sum(weights)))
    least = 1 if total - largest >= amount - 1 else 0
    given, spare = [largest] + [least] * (amount - 1), total - largest - least * (amount - 1)
    while spare > 0:
        free = [i for i in range(1, amount) if given[i] < largest] or [i for i in range(1, amount) if given[i] < limit]
        whole, left = sum([weights[i] for i in free]), spare
        for i in free:
            addition = min(limit - given[i], max(1, left * weights[i] // whole), spare)
            given[i] = given[i] + addition
            spare = spare - addition
    return np.array(given)


def normal_values(rng, shape, spread, most, shards=(), held_as=jnp.bfloat16):
    loudness = level_of(rng, shape, shards, -0.22, 0.18) if shards else 1.0
    entries = jax.random.normal(rng, shape, jnp.float32) * spread * loudness
    return jnp.minimum(jnp.maximum(entries, -most), most).astype(held_as)


def heavy_noise(stream_key, shape, deviation, bound, split, heavy, kind=jnp.bfloat16):
    entries = deviation * jax.random.normal(stream_key, shape, jnp.float32)
    if split:
        entries = entries * level_of(stream_key, shape, split, -0.22, 0.18)
    return jnp.clip(raised(entries, jax.random.fold_in(stream_key, 3), *heavy), -bound, bound).astype(kind)


def setup_inputs(seed: int = 0) -> dict:
    key_of = jax.random.split(jax.random.key(seed), 15)
    moe_in = normal_values(key_of[0], (TOKENS, D), 1.0, 6.0, ((0, 8), (1, 4)))
    cotangent = heavy_noise(key_of[1], (TOKENS, D), 1.0, 6.0, ((0, 8), (1, 4)), (0, 1, 8, 2.0))
    routes_keys = jax.random.split(jax.random.fold_in(key_of[2], 1), TOKENS // TOK_DEV)
    routes_turns = jax.random.permutation(jax.random.fold_in(key_of[2], 3), TOKENS // TOK_DEV)
    routes = jax.vmap(lambda own, number: routed_block(jax.random.fold_in(key_of[2], 2), own, number, TOK_DEV, EXPERTS, TOP, CAP, 2))(routes_keys, routes_turns).reshape((TOKENS, TOP))
    route_weight = jnp.clip(0.2 + 0.8 * jax.random.uniform(key_of[3], (TOKENS, TOP), jnp.float32) ** level_of(key_of[3], (TOKENS, TOP), ((0, 8),), -0.2, 0.2), 0.2, 1.0)
    w_gate = normal_values(key_of[4], (EXPERTS, FF_E, D), D ** -0.5, 0.125, ((0, 8), (1, 4)))
    w_up = normal_values(key_of[5], (EXPERTS, FF_E, D), D ** -0.5, 0.125, ((0, 8), (1, 4)))
    w_down = normal_values(key_of[6], (EXPERTS, FF_E, D), FF_E ** -0.5, 0.09375, ((0, 8), (1, 4)))
    conv_pre = normal_values(key_of[7], (TOKENS, D), 1.0, 6.0, ((0, 8), (1, 4)))
    norm_mean = normal_values(key_of[8], (TOKENS,), 0.5, 3.0, ((0, 8),), jnp.float32)
    norm_rstd = jnp.clip(jnp.exp(math.log(2.0) - 1.3862944 * jax.random.uniform(key_of[9], (TOKENS,), jnp.float32) ** level_of(key_of[9], (TOKENS,), ((0, 8),), -0.2, 0.2)), 0.5, 2.0)
    ln_gain = jnp.clip(1.0 + 0.18 * jax.random.normal(key_of[10], (D,), jnp.float32), 0.1, 1.9)
    ln_shift = normal_values(key_of[11], (D,), 0.5, 3.0, ((0, 4),), jnp.float32)
    taps = normal_values(key_of[12], (KW, D), KW ** -0.5, 1.0, ((1, 4),), jnp.float32)
    w_proj = normal_values(key_of[13], (D, D), D ** -0.5, 0.125, ((0, 8), (1, 4)))
    return {"moe_in": moe_in, "cotangent": cotangent, "routes": routes, "route_weight": route_weight, "w_gate": w_gate, "w_up": w_up, "w_down": w_down, "conv_pre": conv_pre, "norm_mean": norm_mean, "norm_rstd": norm_rstd, "ln_gain": ln_gain, "ln_shift": ln_shift, "taps": taps, "w_proj": w_proj}


def silu_slope(pre_value, sigmoid_value):
    return sigmoid_value * (1.0 + pre_value * (1.0 - sigmoid_value))


def expert_backward(packed):
    expert_rows, routed_rows, gate_weight, up_weight, down_weight = packed
    gate_pre = lax.dot_general(expert_rows, gate_weight, (((1,), (1,)), ((), ())), preferred_element_type=jnp.float32)
    up_pre = lax.dot_general(expert_rows, up_weight, (((1,), (1,)), ((), ())), preferred_element_type=jnp.float32)
    gate_sigmoid = jax.nn.sigmoid(gate_pre)
    gate_active = gate_pre * gate_sigmoid
    hidden = (gate_active * up_pre).astype(jnp.bfloat16)
    hidden_grad = lax.dot_general(routed_rows, down_weight, (((1,), (1,)), ((), ())), preferred_element_type=jnp.float32)
    grad_down = lax.dot_general(hidden, routed_rows, (((0,), (0,)), ((), ())), preferred_element_type=jnp.float32).astype(jnp.bfloat16)
    gate_grad = (hidden_grad * up_pre * silu_slope(gate_pre, gate_sigmoid)).astype(jnp.bfloat16)
    up_grad = (hidden_grad * gate_active).astype(jnp.bfloat16)
    grad_up = lax.dot_general(up_grad, expert_rows, (((0,), (0,)), ((), ())), preferred_element_type=jnp.float32).astype(jnp.bfloat16)
    row_count = expert_rows.shape[0]
    block_width = gate_weight.shape[0] // N_TP
    gate_blocks = gate_grad.astype(jnp.float32).reshape(row_count, N_TP, block_width)
    up_blocks = up_grad.astype(jnp.float32).reshape(row_count, N_TP, block_width)
    gate_wblocks = gate_weight.astype(jnp.float32).reshape(N_TP, block_width, D)
    up_wblocks = up_weight.astype(jnp.float32).reshape(N_TP, block_width, D)
    partial_rows = jnp.einsum("rbf,bfd->rbd", gate_blocks, gate_wblocks) + jnp.einsum("rbf,bfd->rbd", up_blocks, up_wblocks)
    partial_low = lax.optimization_barrier(partial_rows.astype(jnp.bfloat16))
    pair_grad = jnp.sum(partial_low.astype(jnp.float32), axis=1).astype(jnp.bfloat16)
    return grad_up, grad_down, pair_grad


def reference(moe_in, cotangent, routes, route_weight, w_gate, w_up, w_down, conv_pre, norm_mean, norm_rstd, ln_gain, ln_shift, taps, w_proj):
    per_expert = N_SP * CAP
    route_count = TOP * TOKENS
    route_ids = routes.reshape(N_SP, TOP * TOK_DEV)
    onehot = (route_ids[:, :, None] == jnp.arange(EXPERTS, dtype=jnp.int32)[None, None, :]).astype(jnp.int32)
    earlier = jnp.cumsum(onehot, axis=1) - onehot
    slot_ids = jnp.sum(earlier * onehot, axis=2)
    sources = jnp.arange(N_SP, dtype=jnp.int32)[:, None]
    targets = (route_ids * per_expert + sources * CAP + slot_ids).reshape(-1).astype(jnp.int32)
    table = jnp.full((EXPERTS * per_expert,), route_count, jnp.int32).at[targets].set(jnp.arange(route_count, dtype=jnp.int32))
    filled = (table < route_count)[:, None]
    route_of_slot = jnp.minimum(table, route_count - 1).astype(jnp.int32)
    routed_all = (route_weight[:, :, None] * cotangent.astype(jnp.float32)[:, None, :]).astype(jnp.bfloat16).reshape(route_count, D)
    zero_value = jnp.zeros((), jnp.bfloat16)
    expert_rows = jnp.where(filled, moe_in[route_of_slot // TOP], zero_value).reshape(EXPERTS, per_expert, D)
    routed_rows = jnp.where(filled, routed_all[route_of_slot], zero_value).reshape(EXPERTS, per_expert, D)
    grad_up, grad_down, pair_grad = lax.map(expert_backward, (expert_rows, routed_rows, w_gate, w_up, w_down))
    returned = pair_grad.reshape(EXPERTS * per_expert, D)[targets].astype(jnp.float32).reshape(TOKENS, TOP, D)
    grad_stream = (cotangent.astype(jnp.float32) + jnp.sum(returned, axis=1)).astype(jnp.bfloat16)
    normed = (conv_pre.astype(jnp.float32) - norm_mean[:, None]) * norm_rstd[:, None]
    pre_act = normed * ln_gain[None, :] + ln_shift[None, :]
    act_sigmoid = jax.nn.sigmoid(pre_act)
    activated = (pre_act * act_sigmoid).astype(jnp.bfloat16)
    act_grad = jnp.dot(grad_stream, w_proj, preferred_element_type=jnp.float32)
    grad_proj = lax.dot_general(grad_stream, activated, (((0,), (0,)), ((), ())), preferred_element_type=jnp.float32)
    normed_grad = act_grad * silu_slope(pre_act, act_sigmoid) * ln_gain[None, :]
    mean_first = jnp.mean(normed_grad, axis=1, keepdims=True)
    mean_second = jnp.mean(normed_grad * normed, axis=1, keepdims=True)
    conv_grad = norm_rstd[:, None] * (normed_grad - mean_first - normed * mean_second)
    padded = jnp.concatenate([conv_grad, jnp.zeros((KW - 1, D), jnp.float32)], axis=0)
    grad_conv = jnp.zeros((TOKENS, D), jnp.float32)
    for lag in range(KW):
        grad_conv = grad_conv + taps[lag][None, :] * padded[lag:lag + TOKENS]
    return grad_up, grad_down, grad_stream, grad_proj, grad_conv.astype(jnp.bfloat16)
```

```python
import functools

import jax
import jax.numpy as jnp
from jax import lax
from jax.experimental import pallas as pl
from jax.experimental.pallas import tpu as pltpu
from jax.sharding import PartitionSpec as P

MESH = pl.DeviceIdType.MESH


def passed_along(value, axis, steps):
    count = lax.axis_size(axis)
    first, last = (max(0, -steps), min(count, count - steps))
    return lax.ppermute(value, axis, [(source, source + steps) for source in range(first, last)])


def silu_slope(pre_value, sigmoid_value):
    return sigmoid_value * (1.0 + pre_value * (1.0 - sigmoid_value))


def expert_backward(expert_rows, routed_rows, gate_weight, up_weight, down_weight):
    gate_pre = lax.dot_general(
        expert_rows, gate_weight, (((1,), (1,)), ((), ())), preferred_element_type=jnp.float32
    )
    up_pre = lax.dot_general(
        expert_rows, up_weight, (((1,), (1,)), ((), ())), preferred_element_type=jnp.float32
    )
    gate_sigmoid = jax.nn.sigmoid(gate_pre)
    gate_active = gate_pre * gate_sigmoid
    hidden = (gate_active * up_pre).astype(jnp.bfloat16)
    hidden_grad = lax.dot_general(
        routed_rows, down_weight, (((1,), (1,)), ((), ())), preferred_element_type=jnp.float32
    )
    gate_grad = (hidden_grad * up_pre * silu_slope(gate_pre, gate_sigmoid)).astype(jnp.bfloat16)
    up_grad = (hidden_grad * gate_active).astype(jnp.bfloat16)
    partial_rows = jnp.dot(gate_grad, gate_weight, preferred_element_type=jnp.float32)
    partial_rows = partial_rows + jnp.dot(up_grad, up_weight, preferred_element_type=jnp.float32)
    return ((hidden, routed_rows, up_grad, expert_rows), partial_rows.astype(jnp.bfloat16))


def places():
    group, lane = (lax.axis_index("sp"), lax.axis_index("tp"))
    return (group, lane, lax.div(lane, 2), lax.rem(lane, 2))


def greet(groups, chips):
    group, lane, chip, core = places()
    barrier = pltpu.get_barrier_semaphore()

    def hello(sp_index, tp_index):
        pl.semaphore_signal(barrier, inc=1, device_id=(sp_index, tp_index), device_id_type=MESH)

    for step in range(1, groups):
        hello(lax.rem(group + step, groups), lane)
    for step in range(1, chips):
        hello(group, lax.rem(chip + step, chips) * 2 + core)
    hello(group, chip * 2 + 1 - core)
    pl.semaphore_wait(barrier, groups + chips - 1)


def aligned(index, size):
    return pl.ds(pl.multiple_of(index * size, size), size)


def spread_kernel(groups, chips, send_ref, out_ref, sp_send, sp_recv, chip_send, chip_recv, core_send, core_recv, own_sem):
    group, lane, chip, core = places()
    rows = send_ref.shape[1] // groups
    width = send_ref.shape[2]
    greet(groups, chips)

    def remote(source, target, sends, recvs, device):
        copy = pltpu.make_async_remote_copy(
            src_ref=source, dst_ref=target, send_sem=sends, recv_sem=recvs,
            device_id=device, device_id_type=MESH,
        )
        copy.start()
        return copy

    def block(owner, lane_index):
        return out_ref.at[:, aligned(owner, rows), aligned(lane_index, width)]

    own = pltpu.make_async_copy(send_ref.at[:, aligned(group, rows)], block(group, lane), own_sem)
    own.start()
    first = []
    for step in range(1, groups):
        target = lax.rem(group + step, groups)
        first.append(remote(
            send_ref.at[:, aligned(target, rows)], block(group, lane),
            sp_send.at[step], sp_recv.at[step], (target, lane),
        ))
    own.wait()
    partner = (group, chip * 2 + 1 - core)
    pending, relays = ([], [])

    def relay(entry):
        copy, owner, peer, step, turn = entry
        copy.wait_recv()
        relays.append(remote(
            block(owner, peer), block(owner, peer),
            core_send.at[step, turn], core_recv.at[step, turn], partner,
        ))

    for step in range(groups):
        owner = lax.rem(group + groups - step, groups)
        if step:
            first[step - 1].wait_recv()
        fresh = []
        for turn in range(1, chips):
            peer_to = lax.rem(chip + turn, chips) * 2 + core
            peer_from = lax.rem(chip + chips - turn, chips) * 2 + core
            copy = remote(
                block(owner, lane), block(owner, lane),
                chip_send.at[step, turn], chip_recv.at[step, turn], (group, peer_to),
            )
            fresh.append((copy, owner, peer_from, step, turn))
        relays.append(remote(
            block(owner, lane), block(owner, lane),
            core_send.at[step, 0], core_recv.at[step, 0], partner,
        ))
        for entry in pending[max(0, len(pending) - chips + 1):]:
            relay(entry)
        pending.extend(fresh)
    for entry in pending[len(pending) - chips + 1:]:
        relay(entry)
    for copy in first:
        copy.wait_send()
    for entry in pending:
        entry[0].wait_send()
    for copy in relays:
        copy.wait()


def spread(send, groups, chips, number):
    pairs, rows, width = send.shape
    dma = pltpu.SemaphoreType.DMA
    return pl.pallas_call(
        functools.partial(spread_kernel, groups, chips),
        out_shape=jax.ShapeDtypeStruct((pairs, rows, width * chips * 2), send.dtype),
        in_specs=[pl.BlockSpec(memory_space=pltpu.VMEM)],
        out_specs=pl.BlockSpec(memory_space=pltpu.VMEM),
        scratch_shapes=[
            dma((groups,)), dma((groups,)),
            dma((groups, chips)), dma((groups, chips)),
            dma((groups, chips)), dma((groups, chips)),
            dma,
        ],
        compiler_params=pltpu.CompilerParams(collective_id=number, has_side_effects=True),
        cost_estimate=pl.CostEstimate(flops=10**10, bytes_accessed=10**6, transcendentals=0),
    )(send)


def collect_kernel(groups, chips, part_ref, out_ref, half, summed, arrived, total, core_send, core_recv, chip_send, chip_recv, sp_send, sp_recv):
    group, lane, chip, core = places()
    rows = part_ref.shape[0] // groups
    width = out_ref.shape[1]
    greet(groups, chips)
    partner = (group, chip * 2 + 1 - core)

    def remote(source, target, sends, recvs, device):
        copy = pltpu.make_async_remote_copy(
            src_ref=source, dst_ref=target, send_sem=sends, recv_sem=recvs,
            device_id=device, device_id_type=MESH,
        )
        copy.start()
        return copy

    swaps = []
    for turn in [*range(1, chips), 0]:
        away = lax.rem(chip + turn, chips)
        swaps.append(remote(
            part_ref.at[:, aligned(away * 2 + 1 - core, width)], half.at[turn],
            core_send.at[turn], core_recv.at[turn], partner,
        ))
    across = []
    for turn in range(1, chips):
        away = lax.rem(chip + turn, chips)
        swaps[turn - 1].wait_recv()
        for step in range(groups):
            owner = lax.rem(group + step + 1, groups)
            here = aligned(owner, rows)
            summed[turn - 1, here, :] = (
                part_ref[here, aligned(away * 2 + core, width)].astype(jnp.float32)
                + half[turn, here, :].astype(jnp.float32)
            ).astype(jnp.bfloat16)
            across.append(remote(
                summed.at[turn - 1, here], arrived.at[turn - 1, here],
                chip_send.at[turn, step], chip_recv.at[turn, step],
                (group, away * 2 + core),
            ))
    swaps[chips - 1].wait_recv()
    homes = []
    for step in range(groups):
        owner = lax.rem(group + step + 1, groups)
        here = aligned(owner, rows)
        value = part_ref[here, aligned(lane, width)].astype(jnp.float32)
        value = value + half[0, here, :].astype(jnp.float32)
        for turn in range(1, chips):
            across[(turn - 1) * groups + step].wait_recv()
            value = value + arrived[turn - 1, here, :].astype(jnp.float32)
        if step < groups - 1:
            total[here, :] = value.astype(jnp.bfloat16)
            homes.append(remote(
                total.at[here], out_ref.at[aligned(group, rows)],
                sp_send.at[step], sp_recv.at[step], (owner, lane),
            ))
        else:
            out_ref[here, :] = value.astype(jnp.bfloat16)
    for copy in swaps + across:
        copy.wait_send()
    for copy in homes:
        copy.wait()


def collect(part, groups, chips, number):
    rows = part.shape[0]
    width = part.shape[1] // (chips * 2)
    dma = pltpu.SemaphoreType.DMA
    others = max(1, chips - 1)
    return pl.pallas_call(
        functools.partial(collect_kernel, groups, chips),
        out_shape=jax.ShapeDtypeStruct((rows, width), part.dtype),
        in_specs=[pl.BlockSpec(memory_space=pltpu.VMEM)],
        out_specs=pl.BlockSpec(memory_space=pltpu.VMEM),
        scratch_shapes=[
            pltpu.VMEM((chips, rows, width), part.dtype),
            pltpu.VMEM((others, rows, width), part.dtype),
            pltpu.VMEM((others, rows, width), part.dtype),
            pltpu.VMEM((rows, width), part.dtype),
            dma((chips,)), dma((chips,)),
            dma((chips, groups)), dma((chips, groups)),
            dma((groups,)), dma((groups,)),
        ],
        compiler_params=pltpu.CompilerParams(collective_id=number, has_side_effects=True),
        cost_estimate=pl.CostEstimate(flops=10**10, bytes_accessed=10**6, transcendentals=0),
    )(part)


def on_device(
    moe_in,
    cotangent,
    routes,
    route_weight,
    w_gate,
    w_up,
    w_down,
    conv_pre,
    norm_mean,
    norm_rstd,
    ln_gain,
    ln_shift,
    taps,
    w_proj,
):
    devices = lax.axis_size("sp")
    chips = lax.axis_size("tp") // 2
    group = lax.axis_index("sp")
    local_tokens = routes.shape[0]
    channels = moe_in.shape[1]
    width = channels * lax.axis_size("tp")
    capacity = (5 * local_tokens // (2 * devices) + 15) // 16 * 16
    normed = (conv_pre.astype(jnp.float32) - norm_mean[:, None]) * norm_rstd[:, None]
    pre_act = normed * ln_gain[None, :] + ln_shift[None, :]
    act_sigmoid = jax.nn.sigmoid(pre_act)
    activated = (pre_act * act_sigmoid).astype(jnp.bfloat16)
    token = jnp.arange(local_tokens, dtype=jnp.int32)
    before = token[:, None] < token[None, :]
    named = (routes[:, 0], routes[:, 1])
    positions = jnp.arange(devices * capacity, dtype=jnp.int32)
    matches, slot_weight = ([], 0.0)
    for choice in range(2):
        mine = named[choice][None, :]
        same = (named[0][:, None] == mine).astype(jnp.int32) + (named[1][:, None] == mine).astype(jnp.int32)
        target = named[choice] * capacity + jnp.sum(jnp.where(before, same, 0), axis=0)
        match = target[None, :] == positions[:, None]
        matches.append(match)
        slot_weight = slot_weight + jnp.sum(jnp.where(match, route_weight[:, choice][None, :], 0.0), axis=1)
    chosen = (matches[0] | matches[1]).astype(jnp.bfloat16)
    send_rows = jnp.dot(chosen, moe_in, preferred_element_type=jnp.float32).astype(jnp.bfloat16)
    send_routed = (
        slot_weight[:, None] * jnp.dot(chosen, cotangent, preferred_element_type=jnp.float32)
    ).astype(jnp.bfloat16)
    send_both = jnp.stack([send_rows, send_routed])
    whole_active = lax.all_gather(activated, "sp", axis=0, tiled=True)
    spread_rows = spread(send_both, devices, chips, 1)
    spread_rows, w_proj = lax.optimization_barrier((spread_rows, w_proj))
    whole_proj = lax.all_gather(w_proj, "sp", axis=0, tiled=True)
    expert_rows, routed_rows = (spread_rows[0], spread_rows[1])
    (hidden, routed_late, up_grad, rows_late), partial_rows = expert_backward(
        expert_rows, routed_rows, w_gate[0], w_up[0], w_down[0]
    )
    returned_after = lax.optimization_barrier((partial_rows, whole_active))
    partial_rows, whole_active = returned_after
    returned = collect(partial_rows, devices, chips, 2)
    picked = lax.dot_general(
        chosen, returned, (((0,), (0,)), ((), ())), preferred_element_type=jnp.float32
    )
    grad_stream = (cotangent.astype(jnp.float32) + picked).astype(jnp.bfloat16)
    mix_grad = lax.all_gather(grad_stream, "tp", axis=1, tiled=True)
    share = width // devices
    pieces = []
    rotated = lax.dynamic_slice_in_dim(
        jnp.concatenate([mix_grad, mix_grad], axis=1), group * share, width, axis=1
    )
    for step in range(devices):
        piece = rotated[:, step * share : (step + 1) * share]
        if step:
            ring = [(source, (source + step) % devices) for source in range(devices)]
            piece = lax.ppermute(piece, "sp", ring)
        pieces.append(piece)
    rotated, hidden, up_grad = lax.optimization_barrier((rotated, hidden, up_grad))
    grad_down = lax.dot_general(
        hidden, routed_late, (((0,), (0,)), ((), ())), preferred_element_type=jnp.float32
    ).astype(jnp.bfloat16)[None]
    grad_up = lax.dot_general(
        up_grad, rows_late, (((0,), (0,)), ((), ())), preferred_element_type=jnp.float32
    ).astype(jnp.bfloat16)[None]
    act_grad = jnp.dot(mix_grad, whole_proj, preferred_element_type=jnp.float32)
    normed_grad = act_grad * silu_slope(pre_act, act_sigmoid) * ln_gain[None, :]
    first_sum, second_sum = lax.psum(
        (jnp.sum(normed_grad, axis=1), jnp.sum(normed_grad * normed, axis=1)), "tp"
    )
    conv_grad = norm_rstd[:, None] * (
        normed_grad - first_sum[:, None] / width - normed * (second_sum[:, None] / width)
    )
    lag_count = taps.shape[0]
    rim_rows = passed_along(conv_grad[: lag_count - 1], "sp", -1)
    extended = jnp.concatenate([conv_grad, rim_rows], axis=0)
    grad_conv = jnp.zeros((local_tokens, channels), jnp.float32)
    for lag in range(lag_count):
        grad_conv = grad_conv + taps[lag][None, :] * extended[lag : lag + local_tokens]
    stacked = jnp.concatenate(pieces[:1] + pieces[:0:-1], axis=0)
    doubled = jnp.concatenate([whole_active, whole_active], axis=0)
    turned = lax.dynamic_slice_in_dim(doubled, group * local_tokens, devices * local_tokens, axis=0)
    grad_proj = lax.dot_general(
        stacked, turned, (((0,), (0,)), ((), ())), preferred_element_type=jnp.float32
    )
    return (grad_up, grad_down, grad_stream, grad_proj, grad_conv.astype(jnp.bfloat16))


def solution(mesh):
    placed = (
        P("sp", "tp"),
        P("sp", "tp"),
        P("sp", None),
        P("sp", None),
        P("sp", "tp", None),
        P("sp", "tp", None),
        P("sp", "tp", None),
        P("sp", "tp"),
        P("sp"),
        P("sp"),
        P("tp"),
        P("tp"),
        P(None, "tp"),
        P("sp", "tp"),
    )
    return jax.shard_map(
        on_device,
        mesh=mesh,
        in_specs=placed,
        out_specs=(
            P("sp", "tp", None),
            P("sp", "tp", None),
            P("sp", "tp"),
            P("sp", "tp"),
            P("sp", "tp"),
        ),
        check_vma=False,
    )
```
